512 devices in a mesh: fs: 64 (over z, y), tp: 8 (over x, core).
Axes of the slice: x: 4, y: 8, z: 8, core: 2. Of those that a mesh axis runs over, the one named last changes fastest.
Arguments:
- inputs: bfloat16 [32768, 2048], P('fs', 'tp'), may hold values from -6 to 6
- value_cotangent: bfloat16 [32768, 2048], P('fs', 'tp'), may hold values from -6 to 6
- first_map: bfloat16 [32768, 2048], P('fs', 'tp'), may hold values from -6 to 6
- second_map: bfloat16 [32768, 2048], P('fs', 'tp'), may hold values from -6 to 6
- lambdas: float32 [16], P('tp'), may hold values from 0.3 to 0.8
- head_gain: float32 [128], replicated, may hold values from 0.1 to 1.9
- output_cotangent: bfloat16 [32768, 2048], P('fs', 'tp'), may hold values from -6 to 6
- value_factor: bfloat16 [2048, 256], replicated, may hold values from -0.125 to 0.125
- output_factor: bfloat16 [2048, 256], replicated, may hold values from -0.125 to 0.125
- value_weight: float32 [2048, 2048], P('fs', 'tp'), may hold values from -0.125 to 0.125
- output_weight: float32 [2048, 2048], P('tp', 'fs'), may hold values from -0.125 to 0.125
- value_moment: float32 [256, 2048], P('fs', 'tp'), may hold values from -6 to 6
- value_second: float32 [256, 2048], P('fs', 'tp'), may hold values from 0.25 to 4
- output_moment: float32 [256, 2048], P('fs', 'tp'), may hold values from -6 to 6
- output_second: float32 [256, 2048], P('fs', 'tp'), may hold values from 0.25 to 4
Outputs:
- value_master: float32 [2048, 2048], P('fs', 'tp')
- output_master: float32 [2048, 2048], P('tp', 'fs')
- value_moment_new: float32 [256, 2048], P('fs', 'tp')
- value_second_new: float32 [256, 2048], P('fs', 'tp')
- output_moment_new: float32 [256, 2048], P('fs', 'tp')
- output_second_new: float32 [256, 2048], P('fs', 'tp')
- value_copy: bfloat16 [2048, 2048], P(None, 'tp')
- output_copy: bfloat16 [2048, 2048], P('tp')
The draws below stay inside these ranges and needn't reach their ends.
All inputs are finite; a program needn't handle non-finite values.
Results may differ from the reference program's by a relative error of at most 0.0027.
Values may be sent and summed in bfloat16 or wider, within the bound.
No kernel may reach another device: no remote copies, remote signals or barrier semaphores. Data moves between devices by JAX's collectives and lax.ppermute only.
A program may use at most 64 MiB of HBM per device.

```python
import math
import jax
import jax.numpy as jnp
from jax import lax

D = 2048
H = 16
VD = 128
R = 256
TOKENS = 32768


def block_scale(own_key, extent, pieces, smallest, high):
    loudness, own = 1.0, jax.random.fold_in(own_key, 6)
    for dim, blocks in pieces:
        draws = jnp.exp(jax.random.uniform(jax.random.fold_in(own, dim), (blocks,), jnp.float32, smallest / len(pieces), high / len(pieces)))
        loudness = loudness * jnp.repeat(draws, extent[dim] // blocks).reshape([-1 if axis == dim else 1 for axis in range(len(extent))])
    return loudness


def scatter_about(key, extent, spread, limit, shards=(), dtype=jnp.bfloat16):
    values = spread * jax.random.normal(key, extent, jnp.float32)
    if shards:
        values = values * block_scale(key, extent, shards, -0.22, 0.18)
    return jnp.clip(values, -limit, limit).astype(dtype)


def setup_inputs(seed: int = 0) -> dict:
    seeds = jax.random.split(jax.random.key(seed), 16)
    inputs = scatter_about(seeds[0], (TOKENS, D), 1.0, 6.0, ((0, 64), (1, 8)))
    value_cotangent = scatter_about(seeds[1], (TOKENS, H * VD), 1.0, 6.0, ((0, 64), (1, 8)))
    first_map = scatter_about(seeds[2], (TOKENS, H * VD), 1.0, 6.0, ((0, 64), (1, 8)))
    second_map = scatter_about(seeds[3], (TOKENS, H * VD), 1.0, 6.0, ((0, 64), (1, 8)))
    lambdas = jnp.clip(0.3 + 0.5 * jax.random.uniform(seeds[4], (H,), jnp.float32) ** block_scale(seeds[4], (H,), ((0, 8),), -0.2, 0.2), 0.3, 0.8)
    head_gain = jnp.clip(1.0 + 0.18 * jax.random.normal(seeds[5], (VD,), jnp.float32), 0.1, 1.9)
    output_cotangent = scatter_about(seeds[6], (TOKENS, D), 1.0, 6.0, ((0, 64), (1, 8)))
    value_factor = scatter_about(seeds[7], (D, R), D ** -0.5, 0.125)
    output_factor = scatter_about(seeds[8], (D, R), D ** -0.5, 0.125)
    value_weight = scatter_about(seeds[9], (D, H * VD), D ** -0.5, 0.125, ((0, 64), (1, 8)), jnp.float32)
    output_weight = scatter_about(seeds[10], (H * VD, D), (H * VD) ** -0.5, 0.125, ((0, 8), (1, 64)), jnp.float32)
    value_moment = scatter_about(seeds[11], (R, H * VD), 1.0, 6.0, ((0, 64), (1, 8)), jnp.float32)
    value_second = jnp.clip(jnp.exp(math.log(4.0) - 2.7725887 * jax.random.uniform(seeds[12], (R, H * VD), jnp.float32) ** block_scale(seeds[12], (R, H * VD), ((0, 64), (1, 8)), -0.2, 0.2)), 0.25, 4.0)
    output_moment = scatter_about(seeds[13], (R, H * VD), 1.0, 6.0, ((0, 64), (1, 8)), jnp.float32)
    output_second = jnp.clip(jnp.exp(math.log(4.0) - 2.7725887 * jax.random.uniform(seeds[14], (R, H * VD), jnp.float32) ** block_scale(seeds[14], (R, H * VD), ((0, 64), (1, 8)), -0.2, 0.2)), 0.25, 4.0)
    return {"inputs": inputs, "value_cotangent": value_cotangent, "first_map": first_map, "second_map": second_map, "lambdas": lambdas, "head_gain": head_gain, "output_cotangent": output_cotangent, "value_factor": value_factor, "output_factor": output_factor, "value_weight": value_weight, "output_weight": output_weight, "value_moment": value_moment, "value_second": value_second, "output_moment": output_moment, "output_second": output_second}


def contract_rows(left, right, precise):
    if precise:
        return lax.dot_general(left, right, (((0,), (0,)), ((), ())), precision=lax.Precision.HIGHEST, preferred_element_type=jnp.float32)
    return lax.dot_general(left, right, (((0,), (0,)), ((), ())), preferred_element_type=jnp.float32)

def reference(inputs, value_cotangent, first_map, second_map, lambdas, head_gain, output_cotangent, value_factor, output_factor, value_weight, output_weight, value_moment, value_second, output_moment, output_second):
    tok_count = inputs.shape[0]
    first = first_map.astype(jnp.float32).reshape(tok_count, H, VD)
    second = second_map.astype(jnp.float32).reshape(tok_count, H, VD)
    difference = first - lambdas[None, :, None] * second
    normed = difference * lax.rsqrt(lax.optimization_barrier(jnp.mean(difference * difference, axis=-1, keepdims=True)) + 1e-06) * head_gain
    heads_out = normed.reshape(tok_count, H * VD).astype(jnp.bfloat16)
    token_scale = 1.0 / math.sqrt(TOKENS)
    grad_value = contract_rows(inputs, value_cotangent, False) * token_scale
    grad_output_t = contract_rows(output_cotangent, heads_out, False) * token_scale
    low_value = contract_rows(value_factor.astype(jnp.float32), grad_value, True)
    low_output = contract_rows(output_factor.astype(jnp.float32), grad_output_t, True)
    value_moment_new = 0.8 * value_moment + 0.2 * low_value
    value_second_new = 0.95 * value_second + 0.05 * low_value * low_value
    output_moment_new = 0.8 * output_moment + 0.2 * low_output
    output_second_new = 0.95 * output_second + 0.05 * low_output * low_output
    direction_value = value_moment_new / (jnp.sqrt(value_second_new) + 1e-08)
    direction_output = output_moment_new / (jnp.sqrt(output_second_new) + 1e-08)
    step_value = jnp.dot(value_factor.astype(jnp.float32), direction_value, precision=lax.Precision.HIGHEST, preferred_element_type=jnp.float32)
    step_output = jnp.dot(output_factor.astype(jnp.float32), direction_output, precision=lax.Precision.HIGHEST, preferred_element_type=jnp.float32)
    value_master = value_weight - 0.05 * step_value
    output_master = output_weight - 0.05 * step_output.T
    return (value_master, output_master, value_moment_new, value_second_new, output_moment_new, output_second_new, value_master.astype(jnp.bfloat16), output_master.astype(jnp.bfloat16))
```

```python
import math

import jax
import jax.numpy as jnp
from jax import lax
from jax.sharding import PartitionSpec as P

F32 = jnp.float32
BF16 = jnp.bfloat16
F16 = jnp.float16

WEIGHT_SCALE = 2.0**18
TOKEN_SCALE = 2.0**4
LOW_SCALE = 2.0**-2
DIRECTION_SCALE = 2.0**8


def dot(left, right, left_dim, right_dim):
    return lax.dot_general(
        left, right, (((left_dim,), (right_dim,)), ((), ())), preferred_element_type=F32
    )


def two_parts(x):
    high = lax.reduce_precision(x, 8, 7)
    return high.astype(BF16), (x - high).astype(BF16)


def dot_two(left, right_parts, left_dim, right_dim):
    high, low = right_parts
    return dot(left, high, left_dim, right_dim) + dot(left, low, left_dim, right_dim)


def copy_for_each(x, axis):
    size = lax.axis_size(axis)
    return lax.all_to_all(jnp.broadcast_to(x[None], (size, *x.shape)), axis, 0, 0, tiled=True)


def normed_heads(first_map, second_map, lambdas, head_gain):
    width = head_gain.shape[0]
    heads = []
    for h in range(lambdas.shape[0]):
        cols = slice(h * width, (h + 1) * width)
        difference = first_map[:, cols].astype(F32) - lambdas[h] * second_map[:, cols].astype(F32)
        mean = jnp.mean(difference * difference, axis=-1, keepdims=True)
        heads.append((difference * lax.rsqrt(mean + 1e-06) * head_gain[None, :]).astype(BF16))
    return jnp.concatenate(heads, axis=1)


def local(
    inputs,
    value_cotangent,
    first_map,
    second_map,
    lambdas,
    head_gain,
    output_cotangent,
    value_factor,
    output_factor,
    value_weight,
    output_weight,
    value_moment,
    value_second,
    output_moment,
    output_second,
):
    tok_rows, cols = inputs.shape
    rank = value_factor.shape[1]
    fs_size, tp_size = lax.axis_size("fs"), lax.axis_size("tp")
    fs_index, tp_index = lax.axis_index("fs"), lax.axis_index("tp")
    width_rows = value_weight.shape[0]

    own_weights = jnp.concatenate([value_weight, output_weight.T], axis=1)
    weights = lax.all_gather((own_weights * WEIGHT_SCALE).astype(F16), "fs", axis=0, tiled=True)

    in_rows = lax.dynamic_slice_in_dim(value_factor, tp_index * cols, cols, 0)
    cot_rows = lax.dynamic_slice_in_dim(output_factor, tp_index * cols, cols, 0)
    projected = jnp.concatenate(
        [dot(inputs, in_rows, 1, 0), dot(output_cotangent, cot_rows, 1, 0)], axis=1
    )
    pieces = (projected * TOKEN_SCALE).astype(F16).reshape(tp_size, -1, 2 * rank)
    pieces = lax.all_to_all(pieces, "tp", 0, 0, tiled=True)
    summed = jnp.sum(pieces.astype(F32), axis=0).astype(F16)
    tokens = copy_for_each(summed, "tp").reshape(tok_rows, 2 * rank).astype(F32)

    heads_out = normed_heads(first_map, second_map, lambdas, head_gain)
    scale = LOW_SCALE / (TOKEN_SCALE * math.sqrt(tok_rows * fs_size))
    token_parts = two_parts(tokens)
    low_value = dot_two(value_cotangent, [p[:, :rank] for p in token_parts], 0, 0)
    low_output = dot_two(heads_out, [p[:, rank:] for p in token_parts], 0, 0)
    partial = jnp.concatenate([low_value.T, low_output.T], axis=1) * scale
    tiles = partial.astype(F16).reshape(fs_size, -1, 2 * cols)
    tiles = lax.all_to_all(tiles, "fs", 0, 0, tiled=True)
    own_rows = jnp.sum(tiles.astype(F32), axis=0) * (1.0 / LOW_SCALE)

    moments = jnp.concatenate([value_moment, output_moment], axis=1)
    seconds = jnp.concatenate([value_second, output_second], axis=1)
    moment_new = 0.8 * moments + 0.2 * own_rows
    second_new = 0.95 * seconds + 0.05 * own_rows * own_rows
    direction = moment_new / (jnp.sqrt(second_new) + 1e-08)

    directions = copy_for_each((direction * DIRECTION_SCALE).astype(F16), "fs")
    parts = two_parts(directions.reshape(rank, 2 * cols).astype(F32))
    value_parts = [p[:, :cols] for p in parts]
    output_parts = [p[:, cols:] for p in parts]
    rate = 0.05 / DIRECTION_SCALE
    value_rows = lax.dynamic_slice_in_dim(value_factor, fs_index * width_rows, width_rows, 0)
    output_rows = lax.dynamic_slice_in_dim(output_factor, fs_index * width_rows, width_rows, 0)
    value_master = value_weight - rate * dot_two(value_rows, value_parts, 1, 0)
    output_master = output_weight - rate * dot_two(output_rows, output_parts, 1, 0).T

    old_value = weights[:, :cols].astype(F32) * (1.0 / WEIGHT_SCALE)
    old_output = weights[:, cols:].T.astype(F32) * (1.0 / WEIGHT_SCALE)
    value_copy = (old_value - rate * dot_two(value_factor, value_parts, 1, 0)).astype(BF16)
    step_output = dot(output_parts[0], output_factor, 0, 1) + dot(output_parts[1], output_factor, 0, 1)
    output_copy = (old_output - rate * step_output).astype(BF16)
    return (
        value_master,
        output_master,
        moment_new[:, :cols],
        second_new[:, :cols],
        moment_new[:, cols:],
        second_new[:, cols:],
        value_copy,
        output_copy,
    )


def solution(mesh):
    in_specs = (
        P("fs", "tp"),
        P("fs", "tp"),
        P("fs", "tp"),
        P("fs", "tp"),
        P("tp"),
        P(),
        P("fs", "tp"),
        P(),
        P(),
        P("fs", "tp"),
        P("tp", "fs"),
        P("fs", "tp"),
        P("fs", "tp"),
        P("fs", "tp"),
        P("fs", "tp"),
    )
    out_specs = (
        P("fs", "tp"),
        P("tp", "fs"),
        P("fs", "tp"),
        P("fs", "tp"),
        P("fs", "tp"),
        P("fs", "tp"),
        P(None, "tp"),
        P("tp", None),
    )
    return jax.shard_map(local, mesh=mesh, in_specs=in_specs, out_specs=out_specs, check_vma=False)
```

```python
import math

import jax
import jax.numpy as jnp
from jax import lax
from jax.experimental import pallas as pl
from jax.experimental.pallas import tpu as pltpu
from jax.sharding import Mesh, PartitionSpec as P

F32 = jnp.float32
BF16 = jnp.bfloat16
F16 = jnp.float16

FS = ("z", "y")
TP = ("x", "core")

WEIGHT_SCALE = 2.0**18
TOKEN_SCALE = 2.0**4
LOW_SCALE = 2.0**-2
DIRECTION_SCALE = 2.0**8

GROUP = 512


def dot(left, right, left_dim, right_dim):
    return lax.dot_general(
        left, right, (((left_dim,), (right_dim,)), ((), ())), preferred_element_type=F32
    )


def two_parts(x):
    high = lax.reduce_precision(x, 8, 7)
    return high.astype(BF16), (x - high).astype(BF16)


def dot_two(left, right_parts, left_dim, right_dim):
    high, low = right_parts
    return dot(left, high, left_dim, right_dim) + dot(left, low, left_dim, right_dim)


def copy_for_each(x, axis):
    size = lax.axis_size(axis)
    return lax.all_to_all(jnp.broadcast_to(x[None], (size, *x.shape)), axis, 0, 0, tiled=True)


def normed_heads(first_map, second_map, lambdas, head_gain):
    width = head_gain.shape[0]
    heads = []
    for h in range(lambdas.shape[0]):
        cols = slice(h * width, (h + 1) * width)
        difference = first_map[:, cols].astype(F32) - lambdas[h] * second_map[:, cols].astype(F32)
        mean = jnp.mean(difference * difference, axis=-1, keepdims=True)
        heads.append((difference * lax.rsqrt(mean + 1e-06) * head_gain[None, :]).astype(BF16))
    return jnp.concatenate(heads, axis=1)


def from_offset(x, dy, dz):
    ny, nz = lax.axis_size("y"), lax.axis_size("z")
    pairs = []
    for z in range(nz):
        for y in range(ny):
            source = ((z + dz) % nz) * ny + (y + dy) % ny
            pairs.append((source, z * ny + y))
    return lax.ppermute(x, FS, pairs)


DOUBLINGS = ((4, 0), (0, 4), (0, 2), (2, 1))
NEIGHBOURS = ((1, 0), (0, 1), (-1, 0))


def gathered_blocks(block):
    ny, nz = lax.axis_size("y"), lax.axis_size("z")
    held, offsets = block[None], [(0, 0)]
    for dy, dz in DOUBLINGS:
        held = jnp.concatenate([held, from_offset(held, dy, dz)], axis=0)
        offsets = offsets + [(y + dy, z + dz) for y, z in offsets]
    quarters, base = [held], list(offsets)
    for dy, dz in NEIGHBOURS:
        quarters.append(from_offset(held, dy, dz))
        offsets = offsets + [(y + dy, z + dz) for y, z in base]
    place = {(y % ny, z % nz): slot for slot, (y, z) in enumerate(offsets)}
    table = jnp.array([[place[y, z] for y in range(ny)] for z in range(nz)], jnp.int32)
    zs = (jnp.arange(nz) - lax.axis_index("z")) % nz
    ys = (jnp.arange(ny) - lax.axis_index("y")) % ny
    slots = table[zs[:, None], ys[None, :]].reshape(-1)
    return jnp.concatenate(quarters, axis=0), slots


def last_kernel(
    slots,
    blocks,
    high,
    low,
    value_factor,
    output_factor,
    own_value_factor,
    own_output_factor,
    value_weight,
    output_weight_t,
    value_copy,
    output_copy,
    value_master,
    output_master_t,
    high_t,
    low_t,
):
    step = pl.program_id(0)
    cols = value_copy.shape[1]
    width_rows = blocks.shape[1]
    rate = 0.05 / DIRECTION_SCALE

    @pl.when(step == 0)
    def _():
        high_t[...] = high[:, cols:].T
        low_t[...] = low[:, cols:].T
        value_master[...] = value_weight[...] - rate * (
            dot(own_value_factor[...], high[:, :cols], 1, 0)
            + dot(own_value_factor[...], low[:, :cols], 1, 0)
        )
        output_master_t[...] = output_weight_t[...] - rate * (
            dot(own_output_factor[...], high_t[...], 1, 1)
            + dot(own_output_factor[...], low_t[...], 1, 1)
        )

    per_step = value_copy.shape[0] // width_rows
    old = jnp.concatenate(
        [blocks[slots[step * per_step + i]] for i in range(per_step)], axis=0
    ) * (1.0 / WEIGHT_SCALE)
    value_step = dot(value_factor[...], high[:, :cols], 1, 0) + dot(
        value_factor[...], low[:, :cols], 1, 0
    )
    value_copy[...] = (old[:, :cols] - rate * value_step).astype(BF16)
    output_step = dot(high_t[...], output_factor[...], 1, 1) + dot(
        low_t[...], output_factor[...], 1, 1
    )
    output_copy[...] = (old[:, cols:].T - rate * output_step).astype(BF16)


def last_step(slots, blocks, high, low, value_factor, output_factor, own_v, own_o, value_weight, output_weight_t):
    width, rank = value_factor.shape
    rows, cols = value_weight.shape
    whole = lambda *shape: pl.BlockSpec(shape, lambda i, s: (0,) * len(shape))
    return pl.pallas_call(
        last_kernel,
        grid_spec=pltpu.PrefetchScalarGridSpec(
            num_scalar_prefetch=1,
            grid=(width // GROUP,),
            in_specs=[
                whole(*blocks.shape),
                whole(*high.shape),
                whole(*low.shape),
                pl.BlockSpec((GROUP, rank), lambda i, s: (i, 0)),
                pl.BlockSpec((GROUP, rank), lambda i, s: (i, 0)),
                whole(*own_v.shape),
                whole(*own_o.shape),
                whole(rows, cols),
                whole(rows, cols),
            ],
            out_specs=[
                pl.BlockSpec((GROUP, cols), lambda i, s: (i, 0)),
                pl.BlockSpec((cols, GROUP), lambda i, s: (0, i)),
                whole(rows, cols),
                whole(rows, cols),
            ],
            scratch_shapes=[
                pltpu.VMEM((cols, rank), BF16),
                pltpu.VMEM((cols, rank), BF16),
            ],
        ),
        out_shape=[
            jax.ShapeDtypeStruct((width, cols), BF16),
            jax.ShapeDtypeStruct((cols, width), BF16),
            jax.ShapeDtypeStruct((rows, cols), F32),
            jax.ShapeDtypeStruct((rows, cols), F32),
        ],
        name="last_step",
    )(slots, blocks, high, low, value_factor, output_factor, own_v, own_o, value_weight, output_weight_t)


def local(
    inputs,
    value_cotangent,
    first_map,
    second_map,
    lambdas,
    head_gain,
    output_cotangent,
    value_factor,
    output_factor,
    value_weight,
    output_weight,
    value_moment,
    value_second,
    output_moment,
    output_second,
):
    tok_rows, cols = inputs.shape
    rank = value_factor.shape[1]
    fs_size, tp_size = lax.axis_size(FS), lax.axis_size(TP)
    fs_index, tp_index = lax.axis_index(FS), lax.axis_index(TP)
    width_rows = value_weight.shape[0]

    output_weight_t = output_weight.T
    own_weights = jnp.concatenate([value_weight, output_weight_t], axis=1)
    with jax.named_scope("weights"):
        blocks, slots = gathered_blocks((own_weights * WEIGHT_SCALE).astype(F16))

    in_rows = lax.dynamic_slice_in_dim(value_factor, tp_index * cols, cols, 0)
    cot_rows = lax.dynamic_slice_in_dim(output_factor, tp_index * cols, cols, 0)
    projected = jnp.concatenate(
        [dot(inputs, in_rows, 1, 0), dot(output_cotangent, cot_rows, 1, 0)], axis=1
    )
    pieces = (projected * TOKEN_SCALE).astype(F16).reshape(tp_size, -1, 2 * rank)
    pieces = lax.all_to_all(pieces, TP, 0, 0, tiled=True)
    summed = jnp.sum(pieces.astype(F32), axis=0).astype(F16)
    tokens = copy_for_each(summed, TP).reshape(tok_rows, 2 * rank).astype(F32)

    heads_out = normed_heads(first_map, second_map, lambdas, head_gain)
    scale = LOW_SCALE / (TOKEN_SCALE * math.sqrt(tok_rows * fs_size))
    token_parts = two_parts(tokens)
    low_value = dot_two(value_cotangent, [p[:, :rank] for p in token_parts], 0, 0)
    low_output = dot_two(heads_out, [p[:, rank:] for p in token_parts], 0, 0)
    partial = jnp.concatenate([low_value.T, low_output.T], axis=1) * scale
    tiles = partial.astype(F16).reshape(fs_size, -1, 2 * cols)
    tiles = lax.all_to_all(tiles, FS, 0, 0, tiled=True)
    own_rows = jnp.sum(tiles.astype(F32), axis=0) * (1.0 / LOW_SCALE)

    moments = jnp.concatenate([value_moment, output_moment], axis=1)
    seconds = jnp.concatenate([value_second, output_second], axis=1)
    moment_new = 0.8 * moments + 0.2 * own_rows
    second_new = 0.95 * seconds + 0.05 * own_rows * own_rows
    direction = moment_new / (jnp.sqrt(second_new) + 1e-08)

    directions = copy_for_each((direction * DIRECTION_SCALE).astype(F16), FS)
    high, low = two_parts(directions.astype(F32).reshape(rank, 2 * cols))
    own_v = lax.dynamic_slice_in_dim(value_factor, fs_index * width_rows, width_rows, 0)
    own_o = lax.dynamic_slice_in_dim(output_factor, fs_index * width_rows, width_rows, 0)
    value_copy, output_copy, value_master, output_master_t = last_step(
        slots, blocks.astype(F32), high, low, value_factor, output_factor, own_v, own_o, value_weight, output_weight_t
    )
    return (
        value_master,
        output_master_t.T,
        moment_new[:, :cols],
        second_new[:, :cols],
        moment_new[:, cols:],
        second_new[:, cols:],
        value_copy,
        output_copy,
    )


def solution(mesh):
    fs, tp = mesh.devices.shape
    fine = Mesh(mesh.devices.reshape(8, fs // 8, tp // 2, 2), (*FS, *TP))
    rows_cols = P(FS, TP)
    in_specs = (rows_cols,) * 4 + (P(TP), P(), rows_cols, P(), P(), rows_cols, P(TP, FS)) + (rows_cols,) * 4
    out_specs = (rows_cols, P(TP, FS)) + (rows_cols,) * 4 + (P(None, TP), P(TP, None))
    return jax.shard_map(local, mesh=fine, in_specs=in_specs, out_specs=out_specs, check_vma=False)
```

```python
import math

import jax
import jax.numpy as jnp
from jax import lax
from jax.experimental import pallas as pl
from jax.experimental.pallas import tpu as pltpu
from jax.sharding import PartitionSpec as P

F32 = jnp.float32
BF16 = jnp.bfloat16
F16 = jnp.float16

WEIGHT_LIMIT = 0.125
DIRECTION_LIMIT = 16.0
TOKEN_SCALE = 2.0**4
LOW_SCALE = 2.0**-2

CENTRE = 2.0**15.5
GROUP = 512
TOKEN_STEPS = 2


def coded(x, limit):
    size = jnp.maximum(jnp.abs(x) * (1.0 / limit), 2.0**-31) * CENTRE
    square = size * size
    fourth = square * square
    power = 1.0 / (fourth * fourth)
    return jnp.where(x < 0, -power, power).astype(BF16)


def decoded(code, limit):
    power = code.astype(F32)
    size = lax.rsqrt(lax.rsqrt(lax.rsqrt(jnp.abs(power)))) * (limit / CENTRE)
    return jnp.where(power < 0, -size, size)


def dot(left, right, left_dim, right_dim):
    return lax.dot_general(
        left, right, (((left_dim,), (right_dim,)), ((), ())), preferred_element_type=F32
    )


def two_parts(x):
    high = lax.reduce_precision(x, 8, 7)
    return high.astype(BF16), (x - high).astype(BF16)


def dot_two(left, right_parts, left_dim, right_dim):
    high, low = right_parts
    return dot(left, high, left_dim, right_dim) + dot(left, low, left_dim, right_dim)


def copy_for_each(x, axis):
    size = lax.axis_size(axis)
    return lax.all_to_all(jnp.broadcast_to(x[None], (size, *x.shape)), axis, 0, 0, tiled=True)


def normed_heads(first_map, second_map, lambdas, head_gain):
    width = head_gain.shape[0]
    heads = []
    for h in range(lambdas.shape[0]):
        cols = slice(h * width, (h + 1) * width)
        difference = first_map[:, cols].astype(F32) - lambdas[h] * second_map[:, cols].astype(F32)
        mean = jnp.mean(difference * difference, axis=-1, keepdims=True)
        heads.append((difference * lax.rsqrt(mean + 1e-06) * head_gain[None, :]).astype(BF16))
    return jnp.concatenate(heads, axis=1)


def project_kernel(place, inputs, cotangent, value_factor, output_factor, pieces):
    rank = value_factor.shape[1]
    rows = pieces.shape[:2]
    pieces[:, :, :rank] = dot(inputs[...], value_factor[...], 1, 0).astype(BF16).reshape(*rows, rank)
    pieces[:, :, rank:] = dot(cotangent[...], output_factor[...], 1, 0).astype(BF16).reshape(*rows, rank)


def project(place, inputs, cotangent, value_factor, output_factor, parts):
    tokens, cols = inputs.shape
    rank = value_factor.shape[1]
    return pl.pallas_call(
        project_kernel,
        grid_spec=pltpu.PrefetchScalarGridSpec(
            num_scalar_prefetch=1,
            grid=(TOKEN_STEPS,),
            in_specs=[
                pl.BlockSpec((tokens // TOKEN_STEPS, cols), lambda i, p: (i, 0)),
                pl.BlockSpec((tokens // TOKEN_STEPS, cols), lambda i, p: (i, 0)),
                pl.BlockSpec((cols, rank), lambda i, p: (p[0], 0)),
                pl.BlockSpec((cols, rank), lambda i, p: (p[0], 0)),
            ],
            out_specs=pl.BlockSpec(
                (parts // TOKEN_STEPS, tokens // parts, 2 * rank), lambda i, p: (i, 0, 0)
            ),
        ),
        out_shape=jax.ShapeDtypeStruct((parts, tokens // parts, 2 * rank), BF16),
        name="project",
    )(place, inputs, cotangent, value_factor, output_factor)


def last_kernel(
    weights,
    directions,
    value_factor,
    output_factor,
    own_value_factor,
    own_output_factor,
    value_weight,
    output_weight_t,
    value_copy,
    output_copy,
    value_master,
    output_master_t,
    high,
    low,
    high_t,
    low_t,
):
    cols = value_copy.shape[1]

    @pl.when(pl.program_id(0) == 0)
    def _():
        value = decoded(directions[:, :cols], 0.05 * DIRECTION_LIMIT)
        upper = value.astype(BF16)
        high[...] = upper
        low[...] = (value - upper.astype(F32)).astype(BF16)
        output = decoded(directions[:, cols:], 0.05 * DIRECTION_LIMIT).T
        upper = output.astype(BF16)
        high_t[...] = upper
        low_t[...] = (output - upper.astype(F32)).astype(BF16)
        value_master[...] = value_weight[...] - (
            dot(own_value_factor[...], high[...], 1, 0) + dot(own_value_factor[...], low[...], 1, 0)
        )
        output_master_t[...] = output_weight_t[...] - (
            dot(own_output_factor[...], high_t[...], 1, 1)
            + dot(own_output_factor[...], low_t[...], 1, 1)
        )

    old = decoded(weights[...], WEIGHT_LIMIT)
    value_step = dot(value_factor[...], high[...], 1, 0) + dot(value_factor[...], low[...], 1, 0)
    value_copy[...] = (old[:, :cols] - value_step).astype(BF16)
    output_step = dot(high_t[...], output_factor[...], 1, 1) + dot(
        low_t[...], output_factor[...], 1, 1
    )
    output_copy[...] = (old[:, cols:].T - output_step).astype(BF16)


def last_step(weights, directions, value_factor, output_factor, own_v, own_o, value_weight, output_weight_t):
    width, rank = value_factor.shape
    rows, cols = value_weight.shape
    whole = lambda *shape: pl.BlockSpec(shape, lambda i: (0,) * len(shape))
    return pl.pallas_call(
        last_kernel,
        grid=(width // GROUP,),
        in_specs=[
            pl.BlockSpec((GROUP, 2 * cols), lambda i: (i, 0)),
            whole(*directions.shape),
            pl.BlockSpec((GROUP, rank), lambda i: (i, 0)),
            pl.BlockSpec((GROUP, rank), lambda i: (i, 0)),
            whole(*own_v.shape),
            whole(*own_o.shape),
            whole(rows, cols),
            whole(rows, cols),
        ],
        out_specs=[
            pl.BlockSpec((GROUP, cols), lambda i: (i, 0)),
            pl.BlockSpec((cols, GROUP), lambda i: (0, i)),
            whole(rows, cols),
            whole(rows, cols),
        ],
        scratch_shapes=[
            pltpu.VMEM((rank, cols), BF16),
            pltpu.VMEM((rank, cols), BF16),
            pltpu.VMEM((cols, rank), BF16),
            pltpu.VMEM((cols, rank), BF16),
        ],
        out_shape=[
            jax.ShapeDtypeStruct((width, cols), BF16),
            jax.ShapeDtypeStruct((cols, width), BF16),
            jax.ShapeDtypeStruct((rows, cols), F32),
            jax.ShapeDtypeStruct((rows, cols), F32),
        ],
        name="last_step",
    )(weights, directions, value_factor, output_factor, own_v, own_o, value_weight, output_weight_t)


def local(
    inputs,
    value_cotangent,
    first_map,
    second_map,
    lambdas,
    head_gain,
    output_cotangent,
    value_factor,
    output_factor,
    value_weight,
    output_weight,
    value_moment,
    value_second,
    output_moment,
    output_second,
):
    tok_rows, cols = inputs.shape
    rank = value_factor.shape[1]
    fs_size, tp_size = lax.axis_size("fs"), lax.axis_size("tp")
    fs_index, tp_index = lax.axis_index("fs"), lax.axis_index("tp")
    width_rows = value_weight.shape[0]

    output_weight_t = output_weight.T
    own_weights = jnp.concatenate([value_weight, output_weight_t], axis=1)
    weights = lax.all_gather(coded(own_weights, WEIGHT_LIMIT), "fs", axis=0, tiled=True)

    place = jnp.full((1,), tp_index, jnp.int32)
    pieces = project(place, inputs, output_cotangent, value_factor, output_factor, tp_size)
    pieces = lax.all_to_all(pieces, "tp", 0, 0, tiled=True)
    summed = (jnp.sum(pieces.astype(F32), axis=0) * TOKEN_SCALE).astype(F16)
    tokens = copy_for_each(summed, "tp").reshape(tok_rows, 2 * rank).astype(F32)

    heads_out = normed_heads(first_map, second_map, lambdas, head_gain)
    scale = LOW_SCALE / (TOKEN_SCALE * math.sqrt(tok_rows * fs_size))
    token_parts = two_parts(tokens)
    low_value = dot_two(value_cotangent, [p[:, :rank] for p in token_parts], 0, 0)
    low_output = dot_two(heads_out, [p[:, rank:] for p in token_parts], 0, 0)
    partial = jnp.concatenate([low_value.T, low_output.T], axis=1) * scale
    tiles = partial.astype(F16).reshape(fs_size, -1, 2 * cols)
    tiles = lax.all_to_all(tiles, "fs", 0, 0, tiled=True)
    own_rows = jnp.sum(tiles.astype(F32), axis=0) * (1.0 / LOW_SCALE)

    moments = jnp.concatenate([value_moment, output_moment], axis=1)
    seconds = jnp.concatenate([value_second, output_second], axis=1)
    moment_new = 0.8 * moments + 0.2 * own_rows
    second_new = 0.95 * seconds + 0.05 * own_rows * own_rows
    direction = moment_new / (jnp.sqrt(second_new) + 1e-08)

    directions = copy_for_each(coded(direction, DIRECTION_LIMIT), "fs").reshape(rank, 2 * cols)
    own_v = lax.dynamic_slice_in_dim(value_factor, fs_index * width_rows, width_rows, 0)
    own_o = lax.dynamic_slice_in_dim(output_factor, fs_index * width_rows, width_rows, 0)
    value_copy, output_copy, value_master, output_master_t = last_step(
        weights, directions, value_factor, output_factor, own_v, own_o, value_weight, output_weight_t
    )
    return (
        value_master,
        output_master_t.T,
        moment_new[:, :cols],
        second_new[:, :cols],
        moment_new[:, cols:],
        second_new[:, cols:],
        value_copy,
        output_copy,
    )


def solution(mesh):
    rows_cols = P("fs", "tp")
    in_specs = (rows_cols,) * 4 + (P("tp"), P(), rows_cols, P(), P(), rows_cols, P("tp", "fs")) + (rows_cols,) * 4
    out_specs = (rows_cols, P("tp", "fs")) + (rows_cols,) * 4 + (P(None, "tp"), P("tp", None))
    return jax.shard_map(local, mesh=mesh, in_specs=in_specs, out_specs=out_specs, check_vma=False)
```

```python
import math

import jax
import jax.numpy as jnp
from jax import lax
from jax.experimental import pallas as pl
from jax.experimental.pallas import tpu as pltpu
from jax.sharding import Mesh, PartitionSpec as P

F32 = jnp.float32
BF16 = jnp.bfloat16
F16 = jnp.float16

FS = ("z_far", "z_high", "z_low", "y_high", "y_low")
Z, Y = FS[:3], FS[3:]

WEIGHT_LIMIT = 0.125
DIRECTION_LIMIT = 16.0
TOKEN_SCALE = 2.0**4
LOW_SCALE = 2.0**-2

CENTRE = 2.0**15.5
GROUP = 512
TOKEN_STEPS = 2
NEAR_Y = 4


def coded(x, limit):
    size = jnp.maximum(jnp.abs(x) * (1.0 / limit), 2.0**-31) * CENTRE
    square = size * size
    fourth = square * square
    power = 1.0 / (fourth * fourth)
    return jnp.where(x < 0, -power, power).astype(BF16)


def decoded(code, limit):
    power = code.astype(F32)
    size = lax.rsqrt(lax.rsqrt(lax.rsqrt(jnp.abs(power)))) * (limit / CENTRE)
    return jnp.where(power < 0, -size, size)


def dot(left, right, left_dim, right_dim):
    return lax.dot_general(
        left, right, (((left_dim,), (right_dim,)), ((), ())), preferred_element_type=F32
    )


def two_parts(x):
    high = lax.reduce_precision(x, 8, 7)
    return high.astype(BF16), (x - high).astype(BF16)


def dot_two(left, right_parts, left_dim, right_dim):
    high, low = right_parts
    return dot(left, high, left_dim, right_dim) + dot(left, low, left_dim, right_dim)


def copy_for_each(x, axis):
    size = lax.axis_size(axis)
    return lax.all_to_all(jnp.broadcast_to(x[None], (size, *x.shape)), axis, 0, 0, tiled=True)


def normed_heads(first_map, second_map, lambdas, head_gain):
    width = head_gain.shape[0]
    heads = []
    for h in range(lambdas.shape[0]):
        cols = slice(h * width, (h + 1) * width)
        difference = first_map[:, cols].astype(F32) - lambdas[h] * second_map[:, cols].astype(F32)
        mean = jnp.mean(difference * difference, axis=-1, keepdims=True)
        heads.append((difference * lax.rsqrt(mean + 1e-06) * head_gain[None, :]).astype(BF16))
    return jnp.concatenate(heads, axis=1)


def from_offset(x, dy, dz):
    nz, ny = lax.axis_size(Z), lax.axis_size(Y)
    pairs = []
    for z in range(nz):
        for y in range(ny):
            pairs.append((((z + dz) % nz) * ny + (y + dy) % ny, z * ny + y))
    return lax.ppermute(x, FS, pairs)


def all_quarters(own):
    return own, from_offset(own, 1, 0), from_offset(own, 0, -1), from_offset(own, -1, 1)


def project_kernel(place, inputs, cotangent, value_factor, output_factor, pieces):
    rank = value_factor.shape[1]
    rows = pieces.shape[:2]
    pieces[:, :, :rank] = dot(inputs[...], value_factor[...], 1, 0).astype(BF16).reshape(*rows, rank)
    pieces[:, :, rank:] = dot(cotangent[...], output_factor[...], 1, 0).astype(BF16).reshape(*rows, rank)


def project(place, inputs, cotangent, value_factor, output_factor, parts):
    tokens, cols = inputs.shape
    rank = value_factor.shape[1]
    return pl.pallas_call(
        project_kernel,
        grid_spec=pltpu.PrefetchScalarGridSpec(
            num_scalar_prefetch=1,
            grid=(TOKEN_STEPS,),
            in_specs=[
                pl.BlockSpec((tokens // TOKEN_STEPS, cols), lambda i, p: (i, 0)),
                pl.BlockSpec((tokens // TOKEN_STEPS, cols), lambda i, p: (i, 0)),
                pl.BlockSpec((cols, rank), lambda i, p: (p[0], 0)),
                pl.BlockSpec((cols, rank), lambda i, p: (p[0], 0)),
            ],
            out_specs=pl.BlockSpec(
                (parts // TOKEN_STEPS, tokens // parts, 2 * rank), lambda i, p: (i, 0, 0)
            ),
        ),
        out_shape=jax.ShapeDtypeStruct((parts, tokens // parts, 2 * rank), BF16),
        name="project",
    )(place, inputs, cotangent, value_factor, output_factor)


def arrange_kernel(place, own, other_y, other_z, others, weights):
    rows = own.shape[2]
    z_size, y_size = place[2], place[3]
    steps = ((own, 0, 0), (other_y, 0, 1), (other_z, -1, 0), (others, 1, 1))
    for quarter, z_step, y_step in steps:
        holder = (place[0] + z_size + z_step) % z_size
        y_low = (place[1] + y_step) % 2
        for near in range(quarter.shape[0]):
            for slot in range(2):
                z_far = (holder // (z_size // 2) + slot) % 2
                z = z_far * (z_size // 2) + near // NEAR_Y * 2 + holder % 2
                y = near % NEAR_Y * 2 + y_low
                at = pl.multiple_of((z * y_size + y) * rows, rows)
                weights[pl.ds(at, rows), :] = decoded(quarter[near, slot], WEIGHT_LIMIT)


def arrange(place, quarters, width):
    cols = quarters[0].shape[-1]
    return pl.pallas_call(
        arrange_kernel,
        grid_spec=pltpu.PrefetchScalarGridSpec(
            num_scalar_prefetch=1,
            grid=(1,),
            in_specs=[pl.BlockSpec(q.shape, lambda i, p: (0,) * 4) for q in quarters],
            out_specs=pl.BlockSpec((width, cols), lambda i, p: (0, 0)),
        ),
        out_shape=jax.ShapeDtypeStruct((width, cols), F32),
        cost_estimate=pl.CostEstimate(flops=60 * width * cols, bytes_accessed=6 * width * cols, transcendentals=0),
        name="arrange",
    )(place, *quarters)


def last_kernel(
    weights,
    directions,
    value_factor,
    output_factor,
    own_value_factor,
    own_output_factor,
    value_weight,
    output_weight_t,
    value_copy,
    output_copy,
    value_master,
    output_master_t,
    high,
    low,
    high_t,
    low_t,
):
    cols = value_copy.shape[1]

    @pl.when(pl.program_id(0) == 0)
    def _():
        whole = decoded(directions[...], 0.05 * DIRECTION_LIMIT).reshape(high.shape[0], -1)
        value = whole[:, :cols]
        upper = value.astype(BF16)
        high[...] = upper
        low[...] = (value - upper.astype(F32)).astype(BF16)
        output = whole[:, cols:].T
        upper = output.astype(BF16)
        high_t[...] = upper
        low_t[...] = (output - upper.astype(F32)).astype(BF16)
        value_master[...] = value_weight[...] - (
            dot(own_value_factor[...], high[...], 1, 0) + dot(own_value_factor[...], low[...], 1, 0)
        )
        output_master_t[...] = output_weight_t[...] - (
            dot(own_output_factor[...], high_t[...], 1, 1)
            + dot(own_output_factor[...], low_t[...], 1, 1)
        )

    value_step = dot(value_factor[...], high[...], 1, 0) + dot(value_factor[...], low[...], 1, 0)
    value_copy[...] = (weights[:, :cols] - value_step).astype(BF16)
    output_step = dot(high_t[...], output_factor[...], 1, 1) + dot(
        low_t[...], output_factor[...], 1, 1
    )
    output_copy[...] = (weights[:, cols:].T - output_step).astype(BF16)


def last_step(weights, directions, value_factor, output_factor, own_v, own_o, value_weight, output_weight_t):
    width, rank = value_factor.shape
    rows, cols = value_weight.shape
    whole = lambda *shape: pl.BlockSpec(shape, lambda i: (0,) * len(shape))
    return pl.pallas_call(
        last_kernel,
        grid=(width // GROUP,),
        in_specs=[
            pl.BlockSpec((GROUP, 2 * cols), lambda i: (i, 0)),
            whole(*directions.shape),
            pl.BlockSpec((GROUP, rank), lambda i: (i, 0)),
            pl.BlockSpec((GROUP, rank), lambda i: (i, 0)),
            whole(*own_v.shape),
            whole(*own_o.shape),
            whole(rows, cols),
            whole(rows, cols),
        ],
        out_specs=[
            pl.BlockSpec((GROUP, cols), lambda i: (i, 0)),
            pl.BlockSpec((cols, GROUP), lambda i: (0, i)),
            whole(rows, cols),
            whole(rows, cols),
        ],
        scratch_shapes=[
            pltpu.VMEM((rank, cols), BF16),
            pltpu.VMEM((rank, cols), BF16),
            pltpu.VMEM((cols, rank), BF16),
            pltpu.VMEM((cols, rank), BF16),
        ],
        out_shape=[
            jax.ShapeDtypeStruct((width, cols), BF16),
            jax.ShapeDtypeStruct((cols, width), BF16),
            jax.ShapeDtypeStruct((rows, cols), F32),
            jax.ShapeDtypeStruct((rows, cols), F32),
        ],
        name="last_step",
    )(weights, directions, value_factor, output_factor, own_v, own_o, value_weight, output_weight_t)


def update(
    inputs,
    value_cotangent,
    first_map,
    second_map,
    lambdas,
    head_gain,
    output_cotangent,
    value_factor,
    output_factor,
    value_weight,
    output_weight,
    value_moment,
    value_second,
    output_moment,
    output_second,
):
    tok_rows, cols = inputs.shape
    rank = value_factor.shape[1]
    fs_size, tp_size = lax.axis_size(FS), lax.axis_size("tp")
    fs_index, tp_index = lax.axis_index(FS), lax.axis_index("tp")
    width_rows = value_weight.shape[0]

    output_weight_t = output_weight.T
    own_weights = jnp.concatenate([value_weight, output_weight_t], axis=1)
    code = coded(own_weights, WEIGHT_LIMIT)

    place = jnp.full((1,), tp_index, jnp.int32)
    pieces = project(place, inputs, output_cotangent, value_factor, output_factor, tp_size)
    far = from_offset(code, 0, lax.axis_size(Z) // 2)
    pieces = lax.all_to_all(pieces, "tp", 0, 0, tiled=True)
    summed = (jnp.sum(pieces.astype(F32), axis=0) * TOKEN_SCALE).astype(F16)
    summed, far = lax.optimization_barrier((summed, far))
    own_quarter = copy_for_each(jnp.stack([code, far]), ("z_high", "y_high")).reshape(-1, 2, *code.shape)
    tokens = lax.all_gather(summed, "tp", axis=0, tiled=True).astype(F32)

    heads_out = normed_heads(first_map, second_map, lambdas, head_gain)
    scale = LOW_SCALE / (TOKEN_SCALE * math.sqrt(tok_rows * fs_size))
    token_parts = two_parts(tokens)
    low_value = dot_two(value_cotangent, [p[:, :rank] for p in token_parts], 0, 0)
    low_output = dot_two(heads_out, [p[:, rank:] for p in token_parts], 0, 0)
    partial = jnp.concatenate([low_value.T, low_output.T], axis=1) * scale
    partial, own_quarter = lax.optimization_barrier((partial, own_quarter))
    weights = all_quarters(own_quarter)
    tiles = partial.astype(F16).reshape(fs_size, -1, 2 * cols)
    tiles = lax.all_to_all(tiles, FS, 0, 0, tiled=True)
    own_rows = jnp.sum(tiles.astype(F32), axis=0) * (1.0 / LOW_SCALE)

    moments = jnp.concatenate([value_moment, output_moment], axis=1)
    seconds = jnp.concatenate([value_second, output_second], axis=1)
    moment_new = 0.8 * moments + 0.2 * own_rows
    second_new = 0.95 * seconds + 0.05 * own_rows * own_rows
    direction = moment_new / (jnp.sqrt(second_new) + 1e-08)

    directions = copy_for_each(coded(direction, DIRECTION_LIMIT), FS)
    own_v = lax.dynamic_slice_in_dim(value_factor, fs_index * width_rows, width_rows, 0)
    own_o = lax.dynamic_slice_in_dim(output_factor, fs_index * width_rows, width_rows, 0)
    parities = [lax.axis_index(Z), lax.axis_index(Y), lax.axis_size(Z), lax.axis_size(Y)]
    at = jnp.stack([jnp.int32(p) for p in parities])
    old = arrange(at, weights, value_factor.shape[0])
    value_copy, output_copy, value_master, output_master_t = last_step(
        old, directions, value_factor, output_factor, own_v, own_o, value_weight, output_weight_t
    )
    return (
        value_master,
        output_master_t.T,
        moment_new[:, :cols],
        second_new[:, :cols],
        moment_new[:, cols:],
        second_new[:, cols:],
        value_copy,
        output_copy,
    )


def solution(mesh):
    fs, tp = mesh.devices.shape
    fine = Mesh(mesh.devices.reshape(2, 2, 2, fs // 16, 2, tp), (*FS, "tp"))
    rows_cols = P(FS, "tp")
    in_specs = (rows_cols,) * 4 + (P("tp"), P(), rows_cols, P(), P(), rows_cols, P("tp", FS)) + (rows_cols,) * 4
    out_specs = (rows_cols, P("tp", FS)) + (rows_cols,) * 4 + (P(None, "tp"), P("tp", None))
    return jax.shard_map(update, mesh=fine, in_specs=in_specs, out_specs=out_specs, check_vma=False)
```

```python
import math

import jax
import jax.numpy as jnp
from jax import lax
from jax.experimental import pallas as pl
from jax.experimental.pallas import tpu as pltpu
from jax.sharding import Mesh, PartitionSpec as P

F32 = jnp.float32
BF16 = jnp.bfloat16
F16 = jnp.float16

FS = ("z_far", "z_high", "z_low", "y_high", "y_low")
Z, Y = FS[:3], FS[3:]

WEIGHT_LIMIT = 0.125
DIRECTION_LIMIT = 16.0
TOKEN_SCALE = 2.0**4
LOW_SCALE = 2.0**-2

CENTRE = 2.0**15.5
GROUP = 512
TOKEN_STEPS = 2
NEAR_Y = 4


def coded(x, limit):
    size = jnp.maximum(jnp.abs(x) * (1.0 / limit), 2.0**-31) * CENTRE
    square = size * size
    fourth = square * square
    power = 1.0 / (fourth * fourth)
    return jnp.where(x < 0, -power, power).astype(BF16)


def decoded(code, limit):
    power = code.astype(F32)
    size = lax.rsqrt(lax.rsqrt(lax.rsqrt(jnp.abs(power)))) * (limit / CENTRE)
    return jnp.where(power < 0, -size, size)


def dot(left, right, left_dim, right_dim):
    return lax.dot_general(
        left, right, (((left_dim,), (right_dim,)), ((), ())), preferred_element_type=F32
    )


def two_parts(x):
    high = lax.reduce_precision(x, 8, 7)
    return high.astype(BF16), (x - high).astype(BF16)


def copy_for_each(x, axis):
    size = lax.axis_size(axis)
    return lax.all_to_all(jnp.broadcast_to(x[None], (size, *x.shape)), axis, 0, 0, tiled=True)


def normed_heads(first_map, second_map, lambdas, head_gain):
    width = head_gain.shape[0]
    heads = []
    for h in range(lambdas.shape[0]):
        cols = slice(h * width, (h + 1) * width)
        difference = first_map[:, cols].astype(F32) - lambdas[h] * second_map[:, cols].astype(F32)
        mean = jnp.mean(difference * difference, axis=-1, keepdims=True)
        heads.append((difference * lax.rsqrt(mean + 1e-06) * head_gain[None, :]).astype(BF16))
    return jnp.concatenate(heads, axis=1)


def from_offset(x, dy, dz):
    nz, ny = lax.axis_size(Z), lax.axis_size(Y)
    pairs = []
    for z in range(nz):
        for y in range(ny):
            pairs.append((((z + dz) % nz) * ny + (y + dy) % ny, z * ny + y))
    return lax.ppermute(x, FS, pairs)


def all_quarters(own):
    return own, from_offset(own, 1, 0), from_offset(own, 0, -1), from_offset(own, -1, 1)


def project_kernel(place, inputs, cotangent, value_factor, output_factor, pieces):
    rank = value_factor.shape[1]
    rows = pieces.shape[:2]
    pieces[:, :, :rank] = dot(inputs[...], value_factor[...], 1, 0).astype(BF16).reshape(*rows, rank)
    pieces[:, :, rank:] = dot(cotangent[...], output_factor[...], 1, 0).astype(BF16).reshape(*rows, rank)


def project(place, inputs, cotangent, value_factor, output_factor, parts):
    tokens, cols = inputs.shape
    rank = value_factor.shape[1]
    return pl.pallas_call(
        project_kernel,
        grid_spec=pltpu.PrefetchScalarGridSpec(
            num_scalar_prefetch=1,
            grid=(TOKEN_STEPS,),
            in_specs=[
                pl.BlockSpec((tokens // TOKEN_STEPS, cols), lambda i, p: (i, 0)),
                pl.BlockSpec((tokens // TOKEN_STEPS, cols), lambda i, p: (i, 0)),
                pl.BlockSpec((cols, rank), lambda i, p: (p[0], 0)),
                pl.BlockSpec((cols, rank), lambda i, p: (p[0], 0)),
            ],
            out_specs=pl.BlockSpec(
                (parts // TOKEN_STEPS, tokens // parts, 2 * rank), lambda i, p: (i, 0, 0)
            ),
        ),
        out_shape=jax.ShapeDtypeStruct((parts, tokens // parts, 2 * rank), BF16),
        name="project",
    )(place, inputs, cotangent, value_factor, output_factor)


def arrange_kernel(place, own, other_y, other_z, others, weights):
    rows = own.shape[2]
    z_size, y_size = place[2], place[3]
    steps = ((own, 0, 0), (other_y, 0, 1), (other_z, -1, 0), (others, 1, 1))
    for quarter, z_step, y_step in steps:
        holder = (place[0] + z_size + z_step) % z_size
        y_low = (place[1] + y_step) % 2
        for near in range(quarter.shape[0]):
            for slot in range(2):
                z_far = (holder // (z_size // 2) + slot) % 2
                z = z_far * (z_size // 2) + near // NEAR_Y * 2 + holder % 2
                y = near % NEAR_Y * 2 + y_low
                at = pl.multiple_of((z * y_size + y) * rows, rows)
                weights[pl.ds(at, rows), :] = decoded(quarter[near, slot], WEIGHT_LIMIT)


def arrange(place, quarters, width):
    cols = quarters[0].shape[-1]
    return pl.pallas_call(
        arrange_kernel,
        grid_spec=pltpu.PrefetchScalarGridSpec(
            num_scalar_prefetch=1,
            grid=(1,),
            in_specs=[pl.BlockSpec(q.shape, lambda i, p: (0,) * 4) for q in quarters],
            out_specs=pl.BlockSpec((width, cols), lambda i, p: (0, 0)),
        ),
        out_shape=jax.ShapeDtypeStruct((width, cols), F32),
        cost_estimate=pl.CostEstimate(flops=60 * width * cols, bytes_accessed=6 * width * cols, transcendentals=0),
        name="arrange",
    )(place, *quarters)


def kept(x):
    return pltpu.with_memory_space_constraint(x, pltpu.VMEM)


def streamed(x):
    return pltpu.with_memory_space_constraint(x, pltpu.HBM)


def last_kernel(
    weights,
    directions,
    value_factor,
    output_factor,
    own_value_factor,
    own_output_factor,
    value_weight,
    output_weight_t,
    value_copy,
    output_copy,
    value_master,
    output_master_t,
    old,
    value_factors,
    output_factors,
    value_rows,
    output_columns,
    in_sems,
    sems,
):
    width, cols = value_rows.shape
    rank = value_factor.shape[1]
    loads = []
    for step in range(width // GROUP):
        rows = pl.ds(step * GROUP, GROUP)
        arrays = ((value_factor, value_factors), (weights, old), (output_factor, output_factors))
        for i, (array, held) in enumerate(arrays):
            loads.append(pltpu.make_async_copy(array.at[rows, :], held.at[rows, :], in_sems.at[i, step]))
            loads[-1].start()
    whole = decoded(directions[...], 0.05 * DIRECTION_LIMIT).reshape(rank, 2 * cols)
    high = whole[:, :cols].astype(BF16)
    low = (whole[:, :cols] - high.astype(F32)).astype(BF16)
    turned = whole[:, cols:].T
    high_t = turned.astype(BF16)
    low_t = (turned - high_t.astype(F32)).astype(BF16)
    copies = []
    for step in range(width // GROUP):
        rows = slice(step * GROUP, (step + 1) * GROUP)
        for load in loads[3 * step : 3 * step + 3]:
            load.wait()
        factor = value_factors[rows, :]
        value_step = dot(factor, high, 1, 0) + dot(factor, low, 1, 0)
        value_rows[rows, :] = (old[rows, :cols] - value_step).astype(BF16)
        copies.append(pltpu.make_async_copy(value_rows.at[rows, :], value_copy.at[rows, :], sems.at[0, step]))
        copies[-1].start()
        factor = output_factors[rows, :]
        output_step = dot(high_t, factor, 1, 1) + dot(low_t, factor, 1, 1)
        output_columns[:, rows] = (old[rows, cols:].T - output_step).astype(BF16)
        copies.append(pltpu.make_async_copy(output_columns.at[:, rows], output_copy.at[:, rows], sems.at[1, step]))
        copies[-1].start()
    factor = own_value_factor[...]
    value_master[...] = value_weight[...] - (dot(factor, high, 1, 0) + dot(factor, low, 1, 0))
    factor = own_output_factor[...]
    output_master_t[...] = output_weight_t[...] - (dot(factor, high_t, 1, 1) + dot(factor, low_t, 1, 1))
    for copy in copies:
        copy.wait()


def last_step(weights, directions, value_factor, output_factor, own_v, own_o, value_weight, output_weight_t):
    width = value_factor.shape[0]
    rows, cols = value_weight.shape
    in_vmem, in_hbm = pl.BlockSpec(memory_space=pltpu.VMEM), pl.BlockSpec(memory_space=pltpu.HBM)
    return pl.pallas_call(
        last_kernel,
        in_specs=[in_hbm, in_vmem, in_hbm, in_hbm] + [in_vmem] * 4,
        out_specs=[in_hbm, in_hbm, in_vmem, in_vmem],
        scratch_shapes=[
            pltpu.VMEM(weights.shape, F32),
            pltpu.VMEM(value_factor.shape, BF16),
            pltpu.VMEM(output_factor.shape, BF16),
            pltpu.VMEM((width, cols), BF16),
            pltpu.VMEM((cols, width), BF16),
            pltpu.SemaphoreType.DMA((3, width // GROUP)),
            pltpu.SemaphoreType.DMA((2, width // GROUP)),
        ],
        out_shape=[
            jax.ShapeDtypeStruct((width, cols), BF16),
            jax.ShapeDtypeStruct((cols, width), BF16),
            jax.ShapeDtypeStruct((rows, cols), F32),
            jax.ShapeDtypeStruct((rows, cols), F32),
        ],
        name="last_step",
    )(
        streamed(weights),
        kept(directions),
        streamed(value_factor),
        streamed(output_factor),
        own_v,
        own_o,
        value_weight,
        output_weight_t,
    )


def update(
    inputs,
    value_cotangent,
    first_map,
    second_map,
    lambdas,
    head_gain,
    output_cotangent,
    value_factor,
    output_factor,
    value_weight,
    output_weight,
    value_moment,
    value_second,
    output_moment,
    output_second,
):
    tok_rows, cols = inputs.shape
    rank = value_factor.shape[1]
    fs_size, tp_size = lax.axis_size(FS), lax.axis_size("tp")
    fs_index, tp_index = lax.axis_index(FS), lax.axis_index("tp")
    width_rows = value_weight.shape[0]

    output_weight_t = output_weight.T
    own_weights = jnp.concatenate([value_weight, output_weight_t], axis=1)
    code = coded(own_weights, WEIGHT_LIMIT)

    place = jnp.full((1,), tp_index, jnp.int32)
    pieces = project(place, inputs, output_cotangent, value_factor, output_factor, tp_size)
    far = from_offset(code, 0, lax.axis_size(Z) // 2)
    pieces = lax.all_to_all(pieces, "tp", 0, 0, tiled=True)
    summed = (jnp.sum(pieces.astype(F32), axis=0) * TOKEN_SCALE).astype(F16)
    summed, far = lax.optimization_barrier((summed, far))
    own_quarter = copy_for_each(jnp.stack([code, far]), ("z_high", "y_high")).reshape(-1, 2, *code.shape)
    tokens = lax.all_gather(summed, "tp", axis=0, tiled=True).astype(F32)

    heads_out = normed_heads(first_map, second_map, lambdas, head_gain)
    scale = LOW_SCALE / (TOKEN_SCALE * math.sqrt(tok_rows * fs_size))
    token_parts = two_parts(tokens)
    low = []
    for side, right in enumerate((value_cotangent, heads_out)):
        columns = slice(side * rank, (side + 1) * rank)
        both = dot(jnp.concatenate([p[:, columns] for p in token_parts], axis=1), right, 0, 0)
        low.append(both[:rank] + both[rank:])
    partial = jnp.concatenate(low, axis=1) * scale
    partial, own_quarter = lax.optimization_barrier((partial, own_quarter))
    weights = all_quarters(own_quarter)
    tiles = partial.astype(F16).reshape(fs_size, -1, 2 * cols)
    tiles = lax.all_to_all(tiles, FS, 0, 0, tiled=True)
    own_rows = jnp.sum(tiles.astype(F32), axis=0) * (1.0 / LOW_SCALE)

    moments = jnp.concatenate([value_moment, output_moment], axis=1)
    seconds = jnp.concatenate([value_second, output_second], axis=1)
    moment_new = 0.8 * moments + 0.2 * own_rows
    second_new = 0.95 * seconds + 0.05 * own_rows * own_rows
    direction = moment_new / (jnp.sqrt(second_new) + 1e-08)

    directions = copy_for_each(coded(direction, DIRECTION_LIMIT), FS)
    own_v = lax.dynamic_slice_in_dim(value_factor, fs_index * width_rows, width_rows, 0)
    own_o = lax.dynamic_slice_in_dim(output_factor, fs_index * width_rows, width_rows, 0)
    parities = [lax.axis_index(Z), lax.axis_index(Y), lax.axis_size(Z), lax.axis_size(Y)]
    at = jnp.stack([jnp.int32(p) for p in parities])
    old = arrange(at, weights, value_factor.shape[0])
    value_copy, output_copy, value_master, output_master_t = last_step(
        old, directions, value_factor, output_factor, own_v, own_o, value_weight, output_weight_t
    )
    return (
        value_master,
        output_master_t.T,
        moment_new[:, :cols],
        second_new[:, :cols],
        moment_new[:, cols:],
        second_new[:, cols:],
        value_copy,
        output_copy,
    )


def solution(mesh):
    fs, tp = mesh.devices.shape
    fine = Mesh(mesh.devices.reshape(2, 2, 2, fs // 16, 2, tp), (*FS, "tp"))
    rows_cols = P(FS, "tp")
    in_specs = (rows_cols,) * 4 + (P("tp"), P(), rows_cols, P(), P(), rows_cols, P("tp", FS)) + (rows_cols,) * 4
    out_specs = (rows_cols, P("tp", FS)) + (rows_cols,) * 4 + (P(None, "tp"), P("tp", None))
    return jax.shard_map(update, mesh=fine, in_specs=in_specs, out_specs=out_specs, check_vma=False)
```

```python
import math

import jax
import jax.numpy as jnp
from jax import lax
from jax.experimental import pallas as pl
from jax.experimental.pallas import tpu as pltpu
from jax.sharding import Mesh, PartitionSpec as P

F32 = jnp.float32
BF16 = jnp.bfloat16
F16 = jnp.float16

FS = ("z_far", "z_high", "z_low", "y_high", "y_low")
Z, Y = FS[:3], FS[3:]

WEIGHT_LIMIT = 0.125
DIRECTION_LIMIT = 16.0
TOKEN_SCALE = 2.0**4
LOW_SCALE = 2.0**-2

CENTRE = 2.0**15.5
GROUP = 512
TOKEN_STEPS = 1
NEAR_Y = 4


def coded(x, limit):
    size = jnp.maximum(jnp.abs(x) * (1.0 / limit), 2.0**-31) * CENTRE
    square = size * size
    fourth = square * square
    power = 1.0 / (fourth * fourth)
    return jnp.where(x < 0, -power, power).astype(BF16)


def decoded(code, limit):
    power = code.astype(F32)
    size = lax.rsqrt(lax.rsqrt(lax.rsqrt(jnp.abs(power)))) * (limit / CENTRE)
    return jnp.where(power < 0, -size, size)


def dot(left, right, left_dim, right_dim):
    return lax.dot_general(
        left, right, (((left_dim,), (right_dim,)), ((), ())), preferred_element_type=F32
    )


def two_parts(x):
    high = lax.reduce_precision(x, 8, 7)
    return high.astype(BF16), (x - high).astype(BF16)


def copy_for_each(x, axis):
    size = lax.axis_size(axis)
    return lax.all_to_all(jnp.broadcast_to(x[None], (size, *x.shape)), axis, 0, 0, tiled=True)


def normed_heads(first_map, second_map, lambdas, head_gain):
    width = head_gain.shape[0]
    heads = []
    for h in range(lambdas.shape[0]):
        cols = slice(h * width, (h + 1) * width)
        difference = first_map[:, cols].astype(F32) - lambdas[h] * second_map[:, cols].astype(F32)
        mean = jnp.mean(difference * difference, axis=-1, keepdims=True)
        heads.append((difference * lax.rsqrt(mean + 1e-06) * head_gain[None, :]).astype(BF16))
    return jnp.concatenate(heads, axis=1)


def from_offset(x, dy, dz):
    nz, ny = lax.axis_size(Z), lax.axis_size(Y)
    pairs = []
    for z in range(nz):
        for y in range(ny):
            pairs.append((((z + dz) % nz) * ny + (y + dy) % ny, z * ny + y))
    return lax.ppermute(x, FS, pairs)


def all_quarters(own):
    others = from_offset(own, -1, 1)
    return own, from_offset(own, 1, 0), from_offset(own, 0, -1), others


def project_kernel(place, inputs, cotangent, value_factor, output_factor, pieces):
    rank = value_factor.shape[1]
    rows = pieces.shape[:2]
    pieces[:, :, :rank] = dot(inputs[...], value_factor[...], 1, 0).astype(BF16).reshape(*rows, rank)
    pieces[:, :, rank:] = dot(cotangent[...], output_factor[...], 1, 0).astype(BF16).reshape(*rows, rank)


def project(place, inputs, cotangent, value_factor, output_factor, parts):
    tokens, cols = inputs.shape
    rank = value_factor.shape[1]
    return pl.pallas_call(
        project_kernel,
        grid_spec=pltpu.PrefetchScalarGridSpec(
            num_scalar_prefetch=1,
            grid=(TOKEN_STEPS,),
            in_specs=[
                pl.BlockSpec((tokens // TOKEN_STEPS, cols), lambda i, p: (i, 0)),
                pl.BlockSpec((tokens // TOKEN_STEPS, cols), lambda i, p: (i, 0)),
                pl.BlockSpec((cols, rank), lambda i, p: (p[0], 0)),
                pl.BlockSpec((cols, rank), lambda i, p: (p[0], 0)),
            ],
            out_specs=pl.BlockSpec(
                (parts // TOKEN_STEPS, tokens // parts, 2 * rank), lambda i, p: (i, 0, 0)
            ),
        ),
        out_shape=jax.ShapeDtypeStruct((parts, tokens // parts, 2 * rank), BF16),
        name="project",
    )(place, inputs, cotangent, value_factor, output_factor)


def arrange_kernel(place, own, other_y, other_z, others, weights):
    rows = own.shape[2]
    z_size, y_size = place[2], place[3]
    steps = ((own, 0, 0), (other_y, 0, 1), (other_z, -1, 0), (others, 1, 1))
    for quarter, z_step, y_step in steps:
        holder = (place[0] + z_size + z_step) % z_size
        y_low = (place[1] + y_step) % 2
        for near in range(quarter.shape[0]):
            for slot in range(2):
                z_far = (holder // (z_size // 2) + slot) % 2
                z = z_far * (z_size // 2) + near // NEAR_Y * 2 + holder % 2
                y = near % NEAR_Y * 2 + y_low
                at = pl.multiple_of((z * y_size + y) * rows, rows)
                weights[pl.ds(at, rows), :] = decoded(quarter[near, slot], WEIGHT_LIMIT)


def arrange(place, quarters, width):
    cols = quarters[0].shape[-1]
    return pl.pallas_call(
        arrange_kernel,
        grid_spec=pltpu.PrefetchScalarGridSpec(
            num_scalar_prefetch=1,
            grid=(1,),
            in_specs=[pl.BlockSpec(q.shape, lambda i, p: (0,) * 4) for q in quarters],
            out_specs=pl.BlockSpec((width, cols), lambda i, p: (0, 0)),
        ),
        out_shape=jax.ShapeDtypeStruct((width, cols), F32),
        cost_estimate=pl.CostEstimate(flops=60 * width * cols, bytes_accessed=6 * width * cols, transcendentals=0),
        name="arrange",
    )(place, *quarters)


def kept(x):
    return pltpu.with_memory_space_constraint(x, pltpu.VMEM)


def streamed(x):
    return pltpu.with_memory_space_constraint(x, pltpu.HBM)


def last_kernel(
    weights,
    directions,
    value_factor,
    output_factor,
    own_value_factor,
    own_output_factor,
    value_weight,
    output_weight_t,
    value_copy,
    output_copy,
    value_master,
    output_master_t,
    old,
    value_factors,
    output_factors,
    value_rows,
    output_columns,
    own_factors,
    own_rows,
    in_sems,
    own_sems,
    sems,
):
    width, cols = value_rows.shape
    rank = value_factor.shape[1]
    own_loads = []
    for i, array in enumerate((own_value_factor, own_output_factor)):
        own_loads.append(pltpu.make_async_copy(array, own_factors.at[i], own_sems.at[0, i]))
        own_loads[-1].start()
    loads = []
    for step in range(width // GROUP):
        rows = pl.ds(step * GROUP, GROUP)
        arrays = ((value_factor, value_factors), (weights, old), (output_factor, output_factors))
        for i, (array, held) in enumerate(arrays):
            loads.append(pltpu.make_async_copy(array.at[rows, :], held.at[rows, :], in_sems.at[i, step]))
            loads[-1].start()
    whole = decoded(directions[...], 0.05 * DIRECTION_LIMIT).reshape(rank, 2 * cols)
    high = whole[:, :cols].astype(BF16)
    low = (whole[:, :cols] - high.astype(F32)).astype(BF16)
    turned = whole[:, cols:].T
    high_t = turned.astype(BF16)
    low_t = (turned - high_t.astype(F32)).astype(BF16)
    copies = []
    for step in range(width // GROUP):
        rows = slice(step * GROUP, (step + 1) * GROUP)
        for load in loads[3 * step : 3 * step + 3]:
            load.wait()
        factor = value_factors[rows, :]
        value_step = dot(factor, high, 1, 0) + dot(factor, low, 1, 0)
        value_rows[rows, :] = (old[rows, :cols] - value_step).astype(BF16)
        copies.append(pltpu.make_async_copy(value_rows.at[rows, :], value_copy.at[rows, :], sems.at[0, step]))
        copies[-1].start()
        factor = output_factors[rows, :]
        output_step = dot(high_t, factor, 1, 1) + dot(low_t, factor, 1, 1)
        output_columns[:, rows] = (old[rows, cols:].T - output_step).astype(BF16)
        copies.append(pltpu.make_async_copy(output_columns.at[:, rows], output_copy.at[:, rows], sems.at[1, step]))
        copies[-1].start()
        if step == 0:
            for load in own_loads:
                load.wait()
            factor = own_factors[0]
            own_rows[0] = value_weight[...] - (dot(factor, high, 1, 0) + dot(factor, low, 1, 0))
            factor = own_factors[1]
            own_rows[1] = output_weight_t[...] - (dot(factor, high_t, 1, 1) + dot(factor, low_t, 1, 1))
            for i, master in enumerate((value_master, output_master_t)):
                copies.append(pltpu.make_async_copy(own_rows.at[i], master, own_sems.at[1, i]))
                copies[-1].start()
    for copy in copies:
        copy.wait()


def last_step(weights, directions, value_factor, output_factor, own_v, own_o, value_weight, output_weight_t):
    width = value_factor.shape[0]
    rows, cols = value_weight.shape
    in_vmem, in_hbm = pl.BlockSpec(memory_space=pltpu.VMEM), pl.BlockSpec(memory_space=pltpu.HBM)
    return pl.pallas_call(
        last_kernel,
        in_specs=[in_hbm, in_vmem, in_hbm, in_hbm, in_hbm, in_hbm, in_vmem, in_vmem],
        out_specs=[in_hbm] * 4,
        scratch_shapes=[
            pltpu.VMEM(weights.shape, F32),
            pltpu.VMEM(value_factor.shape, BF16),
            pltpu.VMEM(output_factor.shape, BF16),
            pltpu.VMEM((width, cols), BF16),
            pltpu.VMEM((cols, width), BF16),
            pltpu.VMEM((2, *own_v.shape), BF16),
            pltpu.VMEM((2, rows, cols), F32),
            pltpu.SemaphoreType.DMA((3, width // GROUP)),
            pltpu.SemaphoreType.DMA((2, 2)),
            pltpu.SemaphoreType.DMA((2, width // GROUP)),
        ],
        out_shape=[
            jax.ShapeDtypeStruct((width, cols), BF16),
            jax.ShapeDtypeStruct((cols, width), BF16),
            jax.ShapeDtypeStruct((rows, cols), F32),
            jax.ShapeDtypeStruct((rows, cols), F32),
        ],
        name="last_step",
    )(
        streamed(weights),
        kept(directions),
        streamed(value_factor),
        streamed(output_factor),
        streamed(own_v),
        streamed(own_o),
        kept(value_weight),
        kept(output_weight_t),
    )


def update(
    inputs,
    value_cotangent,
    first_map,
    second_map,
    lambdas,
    head_gain,
    output_cotangent,
    value_factor,
    output_factor,
    value_weight,
    output_weight,
    value_moment,
    value_second,
    output_moment,
    output_second,
):
    tok_rows, cols = inputs.shape
    rank = value_factor.shape[1]
    fs_size, tp_size = lax.axis_size(FS), lax.axis_size("tp")
    fs_index, tp_index = lax.axis_index(FS), lax.axis_index("tp")
    width_rows = value_weight.shape[0]

    output_weight_t = output_weight.T
    own_weights = jnp.concatenate([value_weight, output_weight_t], axis=1)
    code = coded(own_weights, WEIGHT_LIMIT)

    place = jnp.full((1,), tp_index, jnp.int32)
    pieces = project(place, inputs, output_cotangent, value_factor, output_factor, tp_size)
    far = from_offset(code, 0, lax.axis_size(Z) // 2)
    pieces = lax.all_to_all(pieces, "tp", 0, 0, tiled=True)
    summed = (jnp.sum(pieces.astype(F32), axis=0) * TOKEN_SCALE).astype(F16)
    summed, far = lax.optimization_barrier((summed, far))
    own_quarter = copy_for_each(jnp.stack([code, far]), ("z_high", "y_high")).reshape(-1, 2, *code.shape)
    tokens = lax.all_gather(summed, "tp", axis=0, tiled=True).astype(F32)

    heads_out = normed_heads(first_map, second_map, lambdas, head_gain)
    scale = LOW_SCALE / (TOKEN_SCALE * math.sqrt(tok_rows * fs_size))
    token_parts = two_parts(tokens)
    low = []
    for side, right in enumerate((value_cotangent, heads_out)):
        columns = slice(side * rank, (side + 1) * rank)
        both = dot(jnp.concatenate([p[:, columns] for p in token_parts], axis=1), right, 0, 0)
        low.append(both[:rank] + both[rank:])
    partial = jnp.concatenate(low, axis=1) * scale
    partial, own_quarter = lax.optimization_barrier((partial, own_quarter))
    weights = all_quarters(own_quarter)
    tiles = partial.astype(F16).reshape(fs_size, -1, 2 * cols)
    tiles = lax.all_to_all(tiles, FS, 0, 0, tiled=True)
    own_rows = jnp.sum(tiles.astype(F32), axis=0) * (1.0 / LOW_SCALE)

    moments = jnp.concatenate([value_moment, output_moment], axis=1)
    seconds = jnp.concatenate([value_second, output_second], axis=1)
    moment_new = 0.8 * moments + 0.2 * own_rows
    second_new = 0.95 * seconds + 0.05 * own_rows * own_rows
    direction = moment_new / (jnp.sqrt(second_new) + 1e-08)

    directions = copy_for_each(coded(direction, DIRECTION_LIMIT), FS)
    own_v = lax.dynamic_slice_in_dim(value_factor, fs_index * width_rows, width_rows, 0)
    own_o = lax.dynamic_slice_in_dim(output_factor, fs_index * width_rows, width_rows, 0)
    parities = [lax.axis_index(Z), lax.axis_index(Y), lax.axis_size(Z), lax.axis_size(Y)]
    at = jnp.stack([jnp.int32(p) for p in parities])
    old = arrange(at, weights, value_factor.shape[0])
    value_copy, output_copy, value_master, output_master_t = last_step(
        old, directions, value_factor, output_factor, own_v, own_o, value_weight, output_weight_t
    )
    return (
        value_master,
        output_master_t.T,
        moment_new[:, :cols],
        second_new[:, :cols],
        moment_new[:, cols:],
        second_new[:, cols:],
        value_copy,
        output_copy,
    )


def solution(mesh):
    fs, tp = mesh.devices.shape
    fine = Mesh(mesh.devices.reshape(2, 2, 2, fs // 16, 2, tp), (*FS, "tp"))
    rows_cols = P(FS, "tp")
    in_specs = (rows_cols,) * 4 + (P("tp"), P(), rows_cols, P(), P(), rows_cols, P("tp", FS)) + (rows_cols,) * 4
    out_specs = (rows_cols, P("tp", FS)) + (rows_cols,) * 4 + (P(None, "tp"), P("tp", None))
    return jax.shard_map(update, mesh=fine, in_specs=in_specs, out_specs=out_specs, check_vma=False)
```
